32 devices in a mesh: sp: 8 (over z, x), tp: 4 (over y, core).
Axes of the slice: x: 2, y: 2, z: 4, core: 2. Of those that a mesh axis runs over, the one named last changes fastest.
Arguments:
- tokens: bfloat16 [2048, 4096], P(('sp', 'tp')), may hold values from -40 to 40, as said below
- query_weight: bfloat16 [2, 4096, 4096], P(None, 'sp', 'tp'), may hold values from -0.09375 to 0.09375
- key_weight: bfloat16 [2, 4096, 512], P(None, 'sp', 'tp'), may hold values from -0.09375 to 0.09375
- value_weight: bfloat16 [2, 4096, 512], P(None, 'sp', 'tp'), may hold values from -0.09375 to 0.09375
- gate_weight: bfloat16 [2, 4096, 4096], P(None, 'sp', 'tp'), may hold values from -0.09375 to 0.09375
- out_weight: bfloat16 [2, 4096, 4096], P(None, 'tp', 'sp'), may hold values from -0.09375 to 0.09375
- sink_logits: float32 [2, 64], replicated, may hold values from 1 to 6
- out_gain: float32 [2, 4096], replicated, may hold values from 0.1 to 1.9
Outputs:
- current: float32 [2048, 4096], P(('sp', 'tp'))
The draws below stay inside these ranges and needn't reach their ends.
Inputs may be any that keep to these rules, and one draw needn't show every extreme that they name: tokens are finite and within -40 to 40.
All inputs are finite; a program needn't handle non-finite values.
Results may differ from the reference program's by a relative error of at most 0.014.
The reference program's roundings to bfloat16 on the way count: a program that leaves them out, or rounds other values in their place, can miss the bound.
Values may be sent and summed in bfloat16 or wider, within the bound.
A program may use at most 128 MiB of HBM per device.

```python
import jax
import jax.numpy as jnp
from jax import lax

D = 4096
HEADS = 64
KV_HEADS = 8
HEAD_DIM = 64
WINDOW = 128
LAYERS = 2
TOKENS = 2048


def draw_tokens(key, part):
    noise = jnp.clip(jax.random.normal(key, (TOKENS, D), jnp.float32), -4.0, 4.0)
    return noise.astype(jnp.bfloat16)


def levels(own_key, dims, split, smallest, high):
    level = 1.0
    for position, blocks in split:
        steps = jax.random.uniform(jax.random.fold_in(jax.random.fold_in(own_key, 6), position), (blocks,), jnp.float32, smallest / len(split), high / len(split))
        level = level * jnp.repeat(jnp.exp(steps), dims[position] // blocks).reshape((-1,) + (1,) * (len(dims) - 1 - position))
    return level


def bell_draw(stream_key, extent, scale, reach, shards=(), kind=jnp.bfloat16):
    values = jax.random.normal(stream_key, extent, jnp.float32) * scale
    if len(shards) > 0:
        values = levels(stream_key, extent, shards, -0.22, 0.18) * values
    return jnp.clip(values, min=-reach, max=reach).astype(kind)


def setup_inputs(seed: int = 0) -> dict:
    seeds = jax.random.split(jax.random.key(seed), 9)
    tokens = draw_tokens(jax.random.fold_in(seeds[8], 71), 0)
    query_weight = bell_draw(seeds[1], (LAYERS, D, HEADS * HEAD_DIM), D ** -0.5, 0.09375, ((1, 8), (2, 4)))
    key_weight = bell_draw(seeds[2], (LAYERS, D, KV_HEADS * HEAD_DIM), D ** -0.5, 0.09375, ((1, 8), (2, 4)))
    value_weight = bell_draw(seeds[3], (LAYERS, D, KV_HEADS * HEAD_DIM), D ** -0.5, 0.09375, ((1, 8), (2, 4)))
    gate_weight = bell_draw(seeds[4], (LAYERS, D, HEADS * HEAD_DIM), D ** -0.5, 0.09375, ((1, 8), (2, 4)))
    out_weight = bell_draw(seeds[5], (LAYERS, HEADS * HEAD_DIM, D), (HEADS * HEAD_DIM) ** -0.5, 0.09375, ((1, 4), (2, 8)))
    sink_logits = jnp.clip(jax.random.uniform(seeds[6], (LAYERS, HEADS), jnp.float32, 1.0, 6.0), 1.0, 6.0)
    out_gain = jnp.clip(1.0 + 0.18 * jax.random.normal(seeds[7], (LAYERS, D), jnp.float32), 0.1, 1.9)
    return {"tokens": tokens, "query_weight": query_weight, "key_weight": key_weight, "value_weight": value_weight, "gate_weight": gate_weight, "out_weight": out_weight, "sink_logits": sink_logits, "out_gain": out_gain}


norm_epsilon = 1e-05
masked_score = -1e+30

def reference(tokens, query_weight, key_weight, value_weight, gate_weight, out_weight, sink_logits, out_gain):
    group_size = HEADS // KV_HEADS
    blocks = TOKENS // WINDOW
    score_scale = HEAD_DIM ** (-0.5)
    current = tokens
    result = None
    for depth_index in range(LAYERS):
        queries = jnp.dot(current, query_weight[depth_index], preferred_element_type=jnp.float32).astype(jnp.bfloat16)
        gate_part = jnp.dot(current, gate_weight[depth_index], preferred_element_type=jnp.float32).astype(jnp.bfloat16)
        key_part = jnp.dot(current, key_weight[depth_index], preferred_element_type=jnp.float32).astype(jnp.bfloat16)
        value_part = jnp.dot(current, value_weight[depth_index], preferred_element_type=jnp.float32).astype(jnp.bfloat16)
        padding = jnp.zeros((WINDOW, KV_HEADS * HEAD_DIM), jnp.bfloat16)
        key_padded = jnp.concatenate([padding, key_part], axis=0).reshape(blocks + 1, WINDOW, KV_HEADS, HEAD_DIM)
        value_padded = jnp.concatenate([padding, value_part], axis=0).reshape(blocks + 1, WINDOW, KV_HEADS, HEAD_DIM)
        key_band = jnp.concatenate([key_padded[:-1], key_padded[1:]], axis=1)
        value_band = jnp.concatenate([value_padded[:-1], value_padded[1:]], axis=1)
        query_blocks = queries.reshape(blocks, WINDOW, KV_HEADS, group_size, HEAD_DIM)
        sink_part = sink_logits[depth_index].astype(jnp.float32).reshape(KV_HEADS, group_size, 1, 1)

        def one_block(inputs):
            query_block, key_block, value_block, number = inputs
            scores = jnp.einsum('qhgd,khd->hgqk', query_block.astype(jnp.float32), key_block.astype(jnp.float32)) * score_scale
            query_pos = number * WINDOW + jnp.arange(WINDOW)
            key_pos = number * WINDOW - WINDOW + jnp.arange(2 * WINDOW)
            distance = query_pos[:, None] - key_pos[None, :]
            visible = (distance >= 0) & (distance < WINDOW) & (key_pos >= 0)[None, :]
            scores = jnp.where(visible[None, None], scores, masked_score)
            highest = jnp.maximum(lax.optimization_barrier(jnp.max(scores, axis=-1, keepdims=True)), sink_part)
            exponent = jnp.exp(scores - highest)
            weights = (exponent / (lax.optimization_barrier(jnp.sum(exponent, axis=-1, keepdims=True)) + jnp.exp(sink_part - highest))).astype(jnp.bfloat16)
            return jnp.einsum('hgqk,khd->qhgd', weights.astype(jnp.float32), value_block.astype(jnp.float32))
        mixture = lax.map(one_block, (query_blocks, key_band, value_band, jnp.arange(blocks)))
        mixture = mixture.reshape(TOKENS, HEADS * HEAD_DIM)
        hidden = (mixture * jax.nn.silu(gate_part.astype(jnp.float32))).astype(jnp.bfloat16)
        summed = jnp.dot(hidden, out_weight[depth_index], preferred_element_type=jnp.float32)
        factor = lax.rsqrt(lax.optimization_barrier(jnp.mean(summed * summed, axis=-1, keepdims=True)) + norm_epsilon)
        result = summed * factor * out_gain[depth_index].astype(jnp.float32)
        current = result.astype(jnp.bfloat16)
    return result
```

```python
import functools

import jax
import jax.numpy as jnp
from jax import lax
from jax.experimental import pallas as pl
from jax.experimental.pallas import tpu as pltpu
from jax.sharding import PartitionSpec as P

HEAD_DIM = 64
WINDOW = 128
LAYERS = 2
GROUP = 8

norm_epsilon = 1e-05
masked_score = -1e30
MESH = pl.DeviceIdType.MESH


def place(nx, ncore):
    sp, tp = lax.axis_index("sp"), lax.axis_index("tp")
    return lax.div(sp, nx), lax.rem(sp, nx), lax.div(tp, ncore), lax.rem(tp, ncore)


def greet(peers):
    barrier = pltpu.get_barrier_semaphore()
    for peer in peers:
        pl.semaphore_signal(barrier, inc=1, device_id=peer, device_id_type=MESH)
    pl.semaphore_wait(barrier, len(peers))


def remote(src, dst, send, recv, peer):
    return pltpu.make_async_remote_copy(
        src_ref=src, dst_ref=dst, send_sem=send, recv_sem=recv, device_id=peer, device_id_type=MESH
    )


def gather_kernel(
    nz, nx, ny, nc, x_ref, a_ref, rows_ref, w_ref,
    own_sem, xz_s, xz_r, xy_s, xy_r, xc_s, xc_r, wz_s, wz_r, wx_s, wx_r,
):
    z, x, y, c = place(nx, nc)
    at = lambda zz, xx, yy, cc: (zz * nx + xx, yy * nc + cc)
    zs = [lax.rem(z + d, nz) for d in range(nz)]
    xs = [lax.rem(x + d, nx) for d in range(nx)]
    ys = [lax.rem(y + d, ny) for d in range(ny)]
    cs = [lax.rem(c + d, nc) for d in range(nc)]
    greet(
        [at(zs[d], x, y, c) for d in range(1, nz)]
        + [at(z, xs[d], y, c) for d in range(1, nx)]
        + [at(z, x, ys[d], c) for d in range(1, ny)]
        + [at(z, x, y, cs[d]) for d in range(1, nc)]
    )
    sent = []

    def go(*args):
        copy = remote(*args)
        copy.start()
        sent.append(copy)

    for d in range(1, nz):
        go(x_ref, rows_ref.at[z, y * nc + c], xz_s.at[d], xz_r.at[d], at(zs[d], x, y, c))
    for d in range(1, nz):
        go(a_ref.at[zs[d]], w_ref.at[z, x], wz_s.at[d], wz_r.at[d], at(zs[d], x, y, c))
    own_rows = pltpu.make_async_copy(x_ref, rows_ref.at[z, y * nc + c], own_sem.at[0])
    own_rows.start()
    own_w = pltpu.make_async_copy(a_ref.at[z], w_ref.at[z, x], own_sem.at[1])
    own_w.start()

    def spread_rows(src, zz, d):
        for e in range(1, ny):
            go(src, rows_ref.at[zz, y * nc + c], xy_s.at[d, e], xy_r.at[d, e], at(z, x, ys[e], c))
        for f in range(1, nc):
            go(src, rows_ref.at[zz, y * nc + c], xc_s.at[d, 0, f], xc_r.at[d, 0, f], at(z, x, y, cs[f]))

    def spread_w(src, zz, d):
        for e in range(1, nx):
            go(src, w_ref.at[zz, x], wx_s.at[d, e], wx_r.at[d, e], at(z, xs[e], y, c))

    spread_w(a_ref.at[z], z, 0)
    spread_rows(x_ref, z, 0)
    froms = [lax.rem(z - d + nz, nz) for d in range(nz)]
    for d in range(1, nz):
        block = rows_ref.at[froms[d], y * nc + c]
        remote(block, block, xz_s.at[d], xz_r.at[d], at(zs[d], x, y, c)).wait_recv()
        spread_rows(block, froms[d], d)
    for d in range(nz):
        for e in range(1, ny):
            yy = lax.rem(y - e + ny, ny)
            block = rows_ref.at[froms[d], yy * nc + c]
            remote(block, block, xy_s.at[d, e], xy_r.at[d, e], at(z, x, ys[e], c)).wait_recv()
            for f in range(1, nc):
                go(block, block, xc_s.at[d, e, f], xc_r.at[d, e, f], at(z, x, y, cs[f]))
    for d in range(1, nz):
        block = w_ref.at[froms[d], x]
        remote(block, block, wz_s.at[d], wz_r.at[d], at(zs[d], x, y, c)).wait_recv()
        spread_w(block, froms[d], d)
    for d in range(nz):
        for e in range(1, nx):
            block = w_ref.at[froms[d], lax.rem(x - e + nx, nx)]
            remote(block, block, wx_s.at[d, e], wx_r.at[d, e], at(z, xs[e], y, c)).wait_recv()
        for e in range(ny):
            for f in range(1, nc):
                yy, cc = lax.rem(y - e + ny, ny), lax.rem(c - f + nc, nc)
                block = rows_ref.at[froms[d], yy * nc + cc]
                remote(block, block, xc_s.at[d, e, f], xc_r.at[d, e, f], at(z, x, y, cs[f])).wait_recv()
    for copy in sent:
        copy.wait_send()
    own_rows.wait()
    own_w.wait()


def gather(nz, nx, ny, nc, ident, rows, blocks):
    dma = pltpu.SemaphoreType.DMA
    return pl.pallas_call(
        functools.partial(gather_kernel, nz, nx, ny, nc),
        out_shape=(
            jax.ShapeDtypeStruct((nz, ny * nc) + rows.shape, rows.dtype),
            jax.ShapeDtypeStruct((nz, nx) + blocks.shape[1:], blocks.dtype),
        ),
        in_specs=[pl.BlockSpec(memory_space=pltpu.VMEM)] * 2,
        out_specs=[pl.BlockSpec(memory_space=pl.ANY)] * 2,
        scratch_shapes=[
            dma((2,)), dma((nz,)), dma((nz,)), dma((nz, ny)), dma((nz, ny)),
            dma((nz, ny, nc)), dma((nz, ny, nc)), dma((nz,)), dma((nz,)), dma((nz, nx)), dma((nz, nx)),
        ],
        compiler_params=pltpu.CompilerParams(collective_id=ident, has_side_effects=True),
        name="gather" + str(ident),
    )(rows, blocks)


def mix_kernel(nz, nx, nc, h_ref, o_ref, all_ref, w_ref, own_sem, hz_s, hz_r, wx_s, wx_r):
    z, x, y, c = place(nx, nc)
    at = lambda zz, xx: (zz * nx + xx, y * nc + c)
    zs = [lax.rem(z + d, nz) for d in range(nz)]
    xs = [lax.rem(x + d, nx) for d in range(nx)]
    greet([at(zs[d], x) for d in range(1, nz)] + [at(z, xs[d]) for d in range(1, nx)])
    wide, deep = h_ref.shape[1], o_ref.shape[1]
    h_at = lambda zz: all_ref.at[:, pl.ds(pl.multiple_of(zz * wide, wide), wide)]
    w_at = lambda xx: w_ref.at[:, pl.ds(pl.multiple_of(xx * deep, deep), deep)]
    copies = []
    for d in range(1, nz):
        copies.append(remote(h_ref, h_at(z), hz_s.at[d], hz_r.at[d], at(zs[d], x)))
    for e in range(1, nx):
        copies.append(remote(o_ref, w_at(x), wx_s.at[e], wx_r.at[e], at(z, xs[e])))
    copies.append(pltpu.make_async_copy(h_ref, h_at(z), own_sem.at[0]))
    copies.append(pltpu.make_async_copy(o_ref, w_at(x), own_sem.at[1]))
    for copy in copies:
        copy.start()
    for copy in copies:
        copy.wait()


def mix(nz, nx, nc, ident, hidden, out_weight):
    dma = pltpu.SemaphoreType.DMA
    return pl.pallas_call(
        functools.partial(mix_kernel, nz, nx, nc),
        out_shape=(
            jax.ShapeDtypeStruct((hidden.shape[0], hidden.shape[1] * nz), hidden.dtype),
            jax.ShapeDtypeStruct((out_weight.shape[0], out_weight.shape[1] * nx), out_weight.dtype),
        ),
        in_specs=[pl.BlockSpec(memory_space=pltpu.VMEM)] * 2,
        out_specs=[pl.BlockSpec(memory_space=pl.ANY)] * 2,
        scratch_shapes=[dma((2,)), dma((nz,)), dma((nz,)), dma((nx,)), dma((nx,))],
        compiler_params=pltpu.CompilerParams(collective_id=ident, has_side_effects=True),
        name="mix" + str(ident),
    )(hidden, out_weight)


def trade_kernel(nz, nx, nc, s_ref, r_ref, own_sem, z_s, z_r):
    z, x, y, c = place(nx, nc)
    at = lambda zz: (zz * nx + x, y * nc + c)
    zs = [lax.rem(z + d, nz) for d in range(nz)]
    greet([at(zs[d]) for d in range(1, nz)])
    copies = [
        remote(s_ref.at[zs[d]], r_ref.at[z], z_s.at[d], z_r.at[d], at(zs[d])) for d in range(1, nz)
    ]
    copies.append(pltpu.make_async_copy(s_ref.at[z], r_ref.at[z], own_sem.at[0]))
    for copy in copies:
        copy.start()
    for copy in copies:
        copy.wait()


def trade(nz, nx, nc, ident, sums):
    dma = pltpu.SemaphoreType.DMA
    return pl.pallas_call(
        functools.partial(trade_kernel, nz, nx, nc),
        out_shape=jax.ShapeDtypeStruct(sums.shape, sums.dtype),
        in_specs=[pl.BlockSpec(memory_space=pltpu.VMEM)],
        out_specs=pl.BlockSpec(memory_space=pltpu.VMEM),
        scratch_shapes=[dma((1,)), dma((nz,)), dma((nz,))],
        compiler_params=pltpu.CompilerParams(collective_id=ident, has_side_effects=True),
        name="trade" + str(ident),
    )(sums)


def per_device(
    nz, nx, ny, nc,
    tokens, query_weight, key_weight, value_weight, gate_weight, out_weight, sink_logits, out_gain,
):
    tp_count = ny * nc
    rows_here, width = tokens.shape
    block_rows = rows_here * tp_count
    heads_tp = query_weight.shape[2] // HEAD_DIM
    heads = heads_tp // nz
    cols = heads * HEAD_DIM
    kv = -(-heads // GROUP)
    kv_cols = kv * HEAD_DIM
    per_kv = heads // kv
    z = lax.div(lax.axis_index("sp"), nx)
    x = lax.rem(lax.axis_index("sp"), nx)
    head_start = lax.axis_index("tp") * heads_tp + z * heads

    offset = jnp.arange(WINDOW + block_rows) - WINDOW
    distance = jnp.arange(block_rows)[:, None] - offset[None, :]
    near = (distance >= 0) & (distance < WINDOW)
    start = (jnp.arange(nz) * nx + x) * block_rows
    visible = near[None] & ((start[:, None] + offset[None, :]) >= 0)[:, None, :]
    score_scale = HEAD_DIM ** (-0.5)
    turn = [(a * nx + b, a * nx + (b + 1) % nx) for a in range(nz) for b in range(nx)]

    def arranged(layer):
        parts = []
        for zz in range(nz):
            kv0 = (zz * heads // GROUP) * HEAD_DIM
            parts.append(
                jnp.concatenate(
                    [
                        query_weight[layer, :, zz * cols : (zz + 1) * cols],
                        gate_weight[layer, :, zz * cols : (zz + 1) * cols],
                        key_weight[layer, :, kv0 : kv0 + kv_cols],
                        value_weight[layer, :, kv0 : kv0 + kv_cols],
                    ],
                    axis=1,
                )
            )
        return jnp.stack(parts)

    current, result = tokens, None
    for layer in range(LAYERS):
        rows, joined = gather(nz, nx, ny, nc, 3 * layer, current, arranged(layer))
        rows = rows.reshape(nz * block_rows, width)
        joined = joined.reshape(width, joined.shape[-1])
        projected = jnp.dot(rows, joined, preferred_element_type=jnp.float32).astype(jnp.bfloat16)
        projected = projected.reshape(nz, block_rows, -1)
        own = projected[:, :, 2 * cols :]
        before = lax.ppermute(own[:, -WINDOW:], "sp", turn)
        later = jnp.concatenate([jnp.zeros_like(before[:1]), before[:-1]], axis=0)
        before = jnp.where(x == 0, later, before)
        nearby = jnp.concatenate([before, own], axis=1)
        queries = projected[:, :, :cols].reshape(nz, block_rows, kv, per_kv, HEAD_DIM)
        gate_part = projected[:, :, cols : 2 * cols]
        key_part = nearby[:, :, :kv_cols].reshape(nz, -1, kv, HEAD_DIM)
        value_part = nearby[:, :, kv_cols:].reshape(nz, -1, kv, HEAD_DIM)
        scores = (
            jnp.einsum("bqhgd,bkhd->bhgqk", queries, key_part, preferred_element_type=jnp.float32)
            * score_scale
        )
        scores = jnp.where(visible[:, None, None], scores, masked_score)
        sink = lax.dynamic_slice_in_dim(sink_logits[layer], head_start, heads, 0)
        sink = sink.reshape(1, kv, per_kv, 1, 1)
        highest = jnp.maximum(jnp.max(scores, axis=-1, keepdims=True), sink)
        exponent = jnp.exp(scores - highest)
        weights = (
            exponent / (jnp.sum(exponent, axis=-1, keepdims=True) + jnp.exp(sink - highest))
        ).astype(jnp.bfloat16)
        mixture = jnp.einsum(
            "bhgqk,bkhd->bqhgd", weights, value_part, preferred_element_type=jnp.float32
        ).reshape(nz, block_rows, cols)
        hidden = (mixture * jax.nn.silu(gate_part.astype(jnp.float32))).astype(jnp.bfloat16)
        hidden, out_cols = mix(
            nz, nx, nc, 3 * layer + 1, hidden.reshape(nz * block_rows, cols), out_weight[layer]
        )
        partial_value = jnp.dot(hidden, out_cols, preferred_element_type=jnp.float32)
        partial_value = partial_value.reshape(nz, tp_count, rows_here, -1)
        summed = lax.psum_scatter(partial_value, "tp", scatter_dimension=1, tiled=False)
        summed = trade(nz, nx, nc, 3 * layer + 2, summed)
        summed = jnp.swapaxes(summed, 0, 1).reshape(rows_here, width)
        factor = lax.rsqrt(jnp.mean(summed * summed, axis=-1, keepdims=True) + norm_epsilon)
        result = summed * factor * out_gain[layer]
        current = result.astype(jnp.bfloat16)
    return result


def solution(mesh):
    sp, tp = mesh.shape["sp"], mesh.shape["tp"]
    nc = 2 if tp % 2 == 0 else 1
    nx = next(n for n in range(1, sp + 1) if sp % n == 0 and n * n * nc >= sp)
    nz = sp // nx
    placed = (
        P(("sp", "tp"), None),
        P(None, "sp", "tp"),
        P(None, "sp", "tp"),
        P(None, "sp", "tp"),
        P(None, "sp", "tp"),
        P(None, "tp", "sp"),
        P(),
        P(),
    )
    return jax.shard_map(
        functools.partial(per_device, nz, nx, tp // nc, nc),
        mesh=mesh, in_specs=placed, out_specs=P(("sp", "tp"), None), check_vma=False,
    )
```

```python
import functools

import jax
import jax.numpy as jnp
from jax import lax
from jax.experimental import pallas as pl
from jax.experimental.pallas import tpu as pltpu
from jax.sharding import PartitionSpec as P

HEAD_DIM = 64
WINDOW = 128
LAYERS = 2
GROUP = 8

norm_epsilon = 1e-05
masked_score = -1e30
MESH = pl.DeviceIdType.MESH


def place(nx, ncore):
    sp, tp = lax.axis_index("sp"), lax.axis_index("tp")
    return lax.div(sp, nx), lax.rem(sp, nx), lax.div(tp, ncore), lax.rem(tp, ncore)


def greet(peers):
    barrier = pltpu.get_barrier_semaphore()
    for peer in peers:
        pl.semaphore_signal(barrier, inc=1, device_id=peer, device_id_type=MESH)
    pl.semaphore_wait(barrier, len(peers))


def remote(src, dst, send, recv, peer):
    return pltpu.make_async_remote_copy(
        src_ref=src, dst_ref=dst, send_sem=send, recv_sem=recv, device_id=peer, device_id_type=MESH
    )


def visits(z, nz, step, act):
    if step == 0:
        act(z, 0)
        return
    pl.when(z >= step)(lambda: act(z - step, 1))
    pl.when(z + step < nz)(lambda: act(z + step, -1))


def chain(z, nz, block, own, send, recv, peer):
    def both(zz, way, use):
        if way >= 0:
            src = own if way == 0 else block(zz)
            copy = remote(src, block(zz), send.at[0, zz], recv.at[zz], peer(z + 1))
            pl.when(z + 1 < nz)(lambda: use(copy))
        if way <= 0:
            src = own if way == 0 else block(zz)
            copy_down = remote(src, block(zz), send.at[1, zz], recv.at[zz], peer(z - 1))
            pl.when(z >= 1)(lambda: use(copy_down))

    return both


def gather_kernel(
    nz, nx, ny, nc, x_ref, a_ref, rows_ref, w_ref,
    own_sem, xz_s, xz_r, xy_s, xy_r, xc_s, xc_r, wz_s, wz_r, wx_s, wx_r,
):
    z, x, y, c = place(nx, nc)
    at = lambda zz, xx, yy, cc: (zz * nx + xx, yy * nc + cc)
    zs = [lax.rem(z + d, nz) for d in range(nz)]
    xs = [lax.rem(x + d, nx) for d in range(nx)]
    ys = [lax.rem(y + d, ny) for d in range(ny)]
    cs = [lax.rem(c + d, nc) for d in range(nc)]
    greet(
        [at(zs[d], x, y, c) for d in range(1, nz)]
        + [at(z, xs[d], y, c) for d in range(1, nx)]
        + [at(z, x, ys[d], c) for d in range(1, ny)]
        + [at(z, x, y, cs[d]) for d in range(1, nc)]
    )
    sent = []
    begin = lambda copy: copy.start()
    end = lambda copy: copy.wait_send()
    spot = lambda zz, yy, cc: rows_ref.at[zz, yy * nc + cc]
    along = chain(z, nz, lambda zz: spot(zz, y, c), x_ref, xz_s, xz_r, lambda zz: at(zz, x, y, c))

    def relay(zz, way, use):
        src = x_ref if way == 0 else spot(zz, y, c)
        for e in range(1, ny):
            use(remote(src, spot(zz, y, c), xy_s.at[zz, e], xy_r.at[zz, e], at(z, x, ys[e], c)))
        for f in range(1, nc):
            use(remote(src, spot(zz, y, c), xc_s.at[zz, 0, f], xc_r.at[zz, 0, f], at(z, x, y, cs[f])))

    def across(zz, use):
        for e in range(1, ny):
            block = spot(zz, lax.rem(y - e + ny, ny), c)
            for f in range(1, nc):
                use(remote(block, block, xc_s.at[zz, e, f], xc_r.at[zz, e, f], at(z, x, y, cs[f])))

    def arrive(zz, way):
        block = spot(zz, y, c)
        remote(block, block, xz_s.at[0, zz], xz_r.at[zz], at(z, x, y, c)).wait_recv()
        along(zz, way, begin)
        relay(zz, way, begin)

    def from_y(zz, way):
        for e in range(1, ny):
            block = spot(zz, lax.rem(y - e + ny, ny), c)
            remote(block, block, xy_s.at[zz, e], xy_r.at[zz, e], at(z, x, ys[e], c)).wait_recv()
        across(zz, begin)

    def from_core(zz, way):
        for e in range(ny):
            for f in range(1, nc):
                block = spot(zz, lax.rem(y - e + ny, ny), lax.rem(c - f + nc, nc))
                remote(block, block, xc_s.at[zz, e, f], xc_r.at[zz, e, f], at(z, x, y, cs[f])).wait_recv()

    def finish(zz, way):
        along(zz, way, end)
        relay(zz, way, end)
        across(zz, end)

    def go(*args):
        copy = remote(*args)
        copy.start()
        sent.append(copy)

    def send_w(d):
        go(a_ref.at[zs[d]], w_ref.at[z, x], wz_s.at[d], wz_r.at[d], at(zs[d], x, y, c))

    def spread_w(src, zz, d):
        for e in range(1, nx):
            go(src, w_ref.at[zz, x], wx_s.at[d, e], wx_r.at[d, e], at(z, xs[e], y, c))

    froms = [lax.rem(z - d + nz, nz) for d in range(nz)]

    def w_arrive(d):
        block = w_ref.at[froms[d], x]
        remote(block, block, wz_s.at[d], wz_r.at[d], at(zs[d], x, y, c)).wait_recv()
        spread_w(block, froms[d], d)

    along(z, 0, begin)
    relay(z, 0, begin)
    spread_w(a_ref.at[z], z, 0)
    own_rows = pltpu.make_async_copy(x_ref, spot(z, y, c), own_sem.at[0])
    own_rows.start()
    own_w = pltpu.make_async_copy(a_ref.at[z], w_ref.at[z, x], own_sem.at[1])
    own_w.start()
    send_w(1)
    for step in range(1, nz):
        visits(z, nz, step, arrive)
        if step + 1 < nz:
            send_w(step + 1)
        w_arrive(step)
    for step in range(nz):
        visits(z, nz, step, from_y)
    for step in range(nz):
        visits(z, nz, step, from_core)
        for e in range(1, nx):
            block = w_ref.at[froms[step], lax.rem(x - e + nx, nx)]
            remote(block, block, wx_s.at[step, e], wx_r.at[step, e], at(z, xs[e], y, c)).wait_recv()
    for step in range(nz):
        visits(z, nz, step, finish)
    for copy in sent:
        copy.wait_send()
    own_rows.wait()
    own_w.wait()


def gather(nz, nx, ny, nc, ident, rows, blocks):
    dma = pltpu.SemaphoreType.DMA
    return pl.pallas_call(
        functools.partial(gather_kernel, nz, nx, ny, nc),
        out_shape=(
            jax.ShapeDtypeStruct((nz, ny * nc) + rows.shape, rows.dtype),
            jax.ShapeDtypeStruct((nz, nx) + blocks.shape[1:], blocks.dtype),
        ),
        in_specs=[pl.BlockSpec(memory_space=pltpu.VMEM)] * 2,
        out_specs=[pl.BlockSpec(memory_space=pl.ANY)] * 2,
        scratch_shapes=[
            dma((2,)), dma((2, nz)), dma((nz,)), dma((nz, ny)), dma((nz, ny)),
            dma((nz, ny, nc)), dma((nz, ny, nc)), dma((nz,)), dma((nz,)), dma((nz, nx)), dma((nz, nx)),
        ],
        compiler_params=pltpu.CompilerParams(collective_id=ident, has_side_effects=True),
        name="gather" + str(ident),
    )(rows, blocks)


def mix_kernel(nz, nx, nc, h_ref, o_ref, all_ref, w_ref, own_sem, hz_s, hz_r, wx_s, wx_r):
    z, x, y, c = place(nx, nc)
    at = lambda zz, xx: (zz * nx + xx, y * nc + c)
    zs = [lax.rem(z + d, nz) for d in range(nz)]
    xs = [lax.rem(x + d, nx) for d in range(nx)]
    greet([at(zs[d], x) for d in range(1, nz)] + [at(z, xs[d]) for d in range(1, nx)])
    wide, deep = h_ref.shape[1], o_ref.shape[1]
    h_at = lambda zz: all_ref.at[:, pl.ds(pl.multiple_of(zz * wide, wide), wide)]
    w_at = lambda xx: w_ref.at[:, pl.ds(pl.multiple_of(xx * deep, deep), deep)]
    along = chain(z, nz, h_at, h_ref, hz_s, hz_r, lambda zz: at(zz, x))
    copies = []
    for e in range(1, nx):
        copies.append(remote(o_ref, w_at(x), wx_s.at[e], wx_r.at[e], at(z, xs[e])))
    copies.append(pltpu.make_async_copy(h_ref, h_at(z), own_sem.at[0]))
    copies.append(pltpu.make_async_copy(o_ref, w_at(x), own_sem.at[1]))
    along(z, 0, lambda copy: copy.start())
    for copy in copies:
        copy.start()

    def arrive(zz, way):
        remote(h_at(zz), h_at(zz), hz_s.at[0, zz], hz_r.at[zz], at(z, x)).wait_recv()
        along(zz, way, lambda copy: copy.start())

    for step in range(1, nz):
        visits(z, nz, step, arrive)
    for copy in copies:
        copy.wait()
    for step in range(nz):
        visits(z, nz, step, lambda zz, way: along(zz, way, lambda copy: copy.wait_send()))


def mix(nz, nx, nc, ident, hidden, out_weight):
    dma = pltpu.SemaphoreType.DMA
    return pl.pallas_call(
        functools.partial(mix_kernel, nz, nx, nc),
        out_shape=(
            jax.ShapeDtypeStruct((hidden.shape[0], hidden.shape[1] * nz), hidden.dtype),
            jax.ShapeDtypeStruct((out_weight.shape[0], out_weight.shape[1] * nx), out_weight.dtype),
        ),
        in_specs=[pl.BlockSpec(memory_space=pltpu.VMEM)] * 2,
        out_specs=[pl.BlockSpec(memory_space=pl.ANY)] * 2,
        scratch_shapes=[dma((2,)), dma((2, nz)), dma((nz,)), dma((nx,)), dma((nx,))],
        compiler_params=pltpu.CompilerParams(collective_id=ident, has_side_effects=True),
        name="mix" + str(ident),
    )(hidden, out_weight)


def settle_kernel(
    nz, nx, ny, nc, p_ref, r_ref, from_c, from_y, half, whole,
    c_s, c_r, y_s, y_r, z_s, z_r,
):
    z, x, y, c = place(nx, nc)
    at = lambda zz, yy, cc: (zz * nx + x, yy * nc + cc)
    zs = [lax.rem(z + d, nz) for d in range(nz)]
    ys = [lax.rem(y + d, ny) for d in range(ny)]
    cs = [lax.rem(c + d, nc) for d in range(nc)]
    greet(
        [at(zs[d], y, c) for d in range(1, nz)]
        + [at(z, ys[d], c) for d in range(1, ny)]
        + [at(z, y, cs[d]) for d in range(1, nc)]
    )
    order = list(range(1, nz)) + [0]
    far = list(range(1, ny)) + [0]
    sent = []

    def go(*args):
        copy = remote(*args)
        copy.start()
        sent.append(copy)

    for d in order:
        for e in far:
            for f in range(1, nc):
                go(
                    p_ref.at[zs[d], ys[e] * nc + cs[f]], from_c.at[d, e, f],
                    c_s.at[d, e, f], c_r.at[d, e, f], at(z, y, cs[f]),
                )
    for d in order:
        for e in far:
            total = p_ref[zs[d], ys[e] * nc + c]
            for f in range(1, nc):
                part = from_c.at[d, e, f]
                remote(part, part, c_s.at[d, e, f], c_r.at[d, e, f], at(z, y, cs[f])).wait_recv()
                total = total + part[...]
            half[d, e] = total
            if e > 0:
                go(half.at[d, e], from_y.at[d, e], y_s.at[d, e], y_r.at[d, e], at(z, ys[e], c))
    for d in order:
        total = half[d, 0]
        for e in range(1, ny):
            part = from_y.at[d, e]
            remote(part, part, y_s.at[d, e], y_r.at[d, e], at(z, ys[e], c)).wait_recv()
            total = total + part[...]
        if d > 0:
            whole[d] = total
            go(whole.at[d], r_ref.at[z], z_s.at[d], z_r.at[d], at(zs[d], y, c))
        else:
            r_ref[z] = total
    for d in range(1, nz):
        block = r_ref.at[lax.rem(z - d + nz, nz)]
        remote(block, block, z_s.at[d], z_r.at[d], at(zs[d], y, c)).wait_recv()
    for copy in sent:
        copy.wait_send()


def settle(nz, nx, ny, nc, ident, partial):
    dma = pltpu.SemaphoreType.DMA
    block = partial.shape[2:]
    return pl.pallas_call(
        functools.partial(settle_kernel, nz, nx, ny, nc),
        out_shape=jax.ShapeDtypeStruct((nz,) + block, partial.dtype),
        in_specs=[pl.BlockSpec(memory_space=pltpu.VMEM)],
        out_specs=pl.BlockSpec(memory_space=pltpu.VMEM),
        scratch_shapes=[
            pltpu.VMEM((nz, ny, nc) + block, partial.dtype),
            pltpu.VMEM((nz, ny) + block, partial.dtype),
            pltpu.VMEM((nz, ny) + block, partial.dtype),
            pltpu.VMEM((nz,) + block, partial.dtype),
            dma((nz, ny, nc)), dma((nz, ny, nc)), dma((nz, ny)), dma((nz, ny)), dma((nz,)), dma((nz,)),
        ],
        compiler_params=pltpu.CompilerParams(collective_id=ident, has_side_effects=True),
        name="settle" + str(ident),
    )(partial)


def per_device(
    nz, nx, ny, nc,
    tokens, query_weight, key_weight, value_weight, gate_weight, out_weight, sink_logits, out_gain,
):
    tp_count = ny * nc
    rows_here, width = tokens.shape
    block_rows = rows_here * tp_count
    heads_tp = query_weight.shape[2] // HEAD_DIM
    heads = heads_tp // nz
    cols = heads * HEAD_DIM
    kv = -(-heads // GROUP)
    kv_cols = kv * HEAD_DIM
    per_kv = heads // kv
    z = lax.div(lax.axis_index("sp"), nx)
    x = lax.rem(lax.axis_index("sp"), nx)
    head_start = lax.axis_index("tp") * heads_tp + z * heads

    offset = jnp.arange(WINDOW + block_rows) - WINDOW
    distance = jnp.arange(block_rows)[:, None] - offset[None, :]
    near = (distance >= 0) & (distance < WINDOW)
    start = (jnp.arange(nz) * nx + x) * block_rows
    visible = near[None] & ((start[:, None] + offset[None, :]) >= 0)[:, None, :]
    score_scale = HEAD_DIM ** (-0.5)
    turn = [(a * nx + b, a * nx + (b + 1) % nx) for a in range(nz) for b in range(nx)]

    def arranged(layer):
        parts = []
        for zz in range(nz):
            kv0 = (zz * heads // GROUP) * HEAD_DIM
            parts.append(
                jnp.concatenate(
                    [
                        query_weight[layer, :, zz * cols : (zz + 1) * cols],
                        gate_weight[layer, :, zz * cols : (zz + 1) * cols],
                        key_weight[layer, :, kv0 : kv0 + kv_cols],
                        value_weight[layer, :, kv0 : kv0 + kv_cols],
                    ],
                    axis=1,
                )
            )
        return jnp.stack(parts)

    current, result = tokens, None
    for layer in range(LAYERS):
        rows, joined = gather(nz, nx, ny, nc, 3 * layer, current, arranged(layer))
        rows = rows.reshape(nz * block_rows, width)
        joined = joined.reshape(width, joined.shape[-1])
        projected = jnp.dot(rows, joined, preferred_element_type=jnp.float32).astype(jnp.bfloat16)
        projected = projected.reshape(nz, block_rows, -1)
        own = projected[:, :, 2 * cols :]
        before = lax.ppermute(own[:, -WINDOW:], "sp", turn)
        later = jnp.concatenate([jnp.zeros_like(before[:1]), before[:-1]], axis=0)
        before = jnp.where(x == 0, later, before)
        nearby = jnp.concatenate([before, own], axis=1)
        queries = projected[:, :, :cols].reshape(nz, block_rows, kv, per_kv, HEAD_DIM)
        gate_part = projected[:, :, cols : 2 * cols]
        key_part = nearby[:, :, :kv_cols].reshape(nz, -1, kv, HEAD_DIM)
        value_part = nearby[:, :, kv_cols:].reshape(nz, -1, kv, HEAD_DIM)
        scores = (
            jnp.einsum("bqhgd,bkhd->bhgqk", queries, key_part, preferred_element_type=jnp.float32)
            * score_scale
        )
        scores = jnp.where(visible[:, None, None], scores, masked_score)
        sink = lax.dynamic_slice_in_dim(sink_logits[layer], head_start, heads, 0)
        sink = sink.reshape(1, kv, per_kv, 1, 1)
        highest = jnp.maximum(jnp.max(scores, axis=-1, keepdims=True), sink)
        exponent = jnp.exp(scores - highest)
        weights = (
            exponent / (jnp.sum(exponent, axis=-1, keepdims=True) + jnp.exp(sink - highest))
        ).astype(jnp.bfloat16)
        mixture = jnp.einsum(
            "bhgqk,bkhd->bqhgd", weights, value_part, preferred_element_type=jnp.float32
        ).reshape(nz, block_rows, cols)
        hidden = (mixture * jax.nn.silu(gate_part.astype(jnp.float32))).astype(jnp.bfloat16)
        hidden, out_cols = mix(
            nz, nx, nc, 3 * layer + 1, hidden.reshape(nz * block_rows, cols), out_weight[layer]
        )
        partial_value = jnp.dot(hidden, out_cols, preferred_element_type=jnp.float32)
        partial_value = partial_value.reshape(nz, tp_count, rows_here, -1)
        summed = settle(nz, nx, ny, nc, 3 * layer + 2, partial_value)
        summed = jnp.swapaxes(summed, 0, 1).reshape(rows_here, width)
        factor = lax.rsqrt(jnp.mean(summed * summed, axis=-1, keepdims=True) + norm_epsilon)
        result = summed * factor * out_gain[layer]
        current = result.astype(jnp.bfloat16)
    return result


def solution(mesh):
    sp, tp = mesh.shape["sp"], mesh.shape["tp"]
    nc = 2 if tp % 2 == 0 else 1
    nx = next(n for n in range(1, sp + 1) if sp % n == 0 and n * n * nc >= sp)
    nz = sp // nx
    placed = (
        P(("sp", "tp"), None),
        P(None, "sp", "tp"),
        P(None, "sp", "tp"),
        P(None, "sp", "tp"),
        P(None, "sp", "tp"),
        P(None, "tp", "sp"),
        P(),
        P(),
    )
    return jax.shard_map(
        functools.partial(per_device, nz, nx, tp // nc, nc),
        mesh=mesh, in_specs=placed, out_specs=P(("sp", "tp"), None), check_vma=False,
    )
```

```python
import functools

import jax
import jax.numpy as jnp
from jax import lax
from jax.experimental import pallas as pl
from jax.experimental.pallas import tpu as pltpu
from jax.sharding import PartitionSpec as P

HEAD_DIM = 64
WINDOW = 128
LAYERS = 2
GROUP = 8

norm_epsilon = 1e-05
masked_score = -1e30
MESH = pl.DeviceIdType.MESH


def place(nx, ncore):
    sp, tp = lax.axis_index("sp"), lax.axis_index("tp")
    return lax.div(sp, nx), lax.rem(sp, nx), lax.div(tp, ncore), lax.rem(tp, ncore)


def greet(peers):
    barrier = pltpu.get_barrier_semaphore()
    for peer in peers:
        pl.semaphore_signal(barrier, inc=1, device_id=peer, device_id_type=MESH)
    pl.semaphore_wait(barrier, len(peers))


def remote(src, dst, send, recv, peer):
    return pltpu.make_async_remote_copy(
        src_ref=src, dst_ref=dst, send_sem=send, recv_sem=recv, device_id=peer, device_id_type=MESH
    )


def visits(z, nz, step, act):
    if step == 0:
        act(z, 0)
        return
    pl.when(z >= step)(lambda: act(z - step, 1))
    pl.when(z + step < nz)(lambda: act(z + step, -1))


def chain(z, nz, block, own, send, recv, peer):
    def both(zz, way, use):
        if way >= 0:
            src = own if way == 0 else block(zz)
            copy = remote(src, block(zz), send.at[0, zz], recv.at[zz], peer(z + 1))
            pl.when(z + 1 < nz)(lambda: use(copy))
        if way <= 0:
            src = own if way == 0 else block(zz)
            copy_down = remote(src, block(zz), send.at[1, zz], recv.at[zz], peer(z - 1))
            pl.when(z >= 1)(lambda: use(copy_down))

    return both


def gather_kernel(
    nz, nx, ny, nc, layer, x_ref, q_ref, g_ref, a_ref, rows_ref, w_ref,
    own_sem, xz_s, xz_r, xy_s, xy_r, xc_s, xc_r, wz_s, wz_r, wx_s, wx_r,
):
    z, x, y, c = place(nx, nc)
    at = lambda zz, xx, yy, cc: (zz * nx + xx, yy * nc + cc)
    zs = [lax.rem(z + d, nz) for d in range(nz)]
    xs = [lax.rem(x + d, nx) for d in range(nx)]
    ys = [lax.rem(y + d, ny) for d in range(ny)]
    cs = [lax.rem(c + d, nc) for d in range(nc)]
    greet(
        [at(zs[d], x, y, c) for d in range(1, nz)]
        + [at(z, xs[d], y, c) for d in range(1, nx)]
        + [at(z, x, ys[d], c) for d in range(1, ny)]
        + [at(z, x, y, cs[d]) for d in range(1, nc)]
    )
    sent = []
    begin = lambda copy: copy.start()
    end = lambda copy: copy.wait_send()
    spot = lambda zz, yy, cc: rows_ref.at[zz, yy * nc + cc]
    along = chain(z, nz, lambda zz: spot(zz, y, c), x_ref, xz_s, xz_r, lambda zz: at(zz, x, y, c))

    def relay(zz, way, use):
        src = x_ref if way == 0 else spot(zz, y, c)
        for e in range(1, ny):
            use(remote(src, spot(zz, y, c), xy_s.at[zz, e], xy_r.at[zz, e], at(z, x, ys[e], c)))
        for f in range(1, nc):
            use(remote(src, spot(zz, y, c), xc_s.at[zz, 0, f], xc_r.at[zz, 0, f], at(z, x, y, cs[f])))

    def across(zz, use):
        for e in range(1, ny):
            block = spot(zz, lax.rem(y - e + ny, ny), c)
            for f in range(1, nc):
                use(remote(block, block, xc_s.at[zz, e, f], xc_r.at[zz, e, f], at(z, x, y, cs[f])))

    def arrive(zz, way):
        block = spot(zz, y, c)
        remote(block, block, xz_s.at[0, zz], xz_r.at[zz], at(z, x, y, c)).wait_recv()
        along(zz, way, begin)
        relay(zz, way, begin)

    def from_y(zz, way):
        for e in range(1, ny):
            block = spot(zz, lax.rem(y - e + ny, ny), c)
            remote(block, block, xy_s.at[zz, e], xy_r.at[zz, e], at(z, x, ys[e], c)).wait_recv()
        across(zz, begin)

    def from_core(zz, way):
        for e in range(ny):
            for f in range(1, nc):
                block = spot(zz, lax.rem(y - e + ny, ny), lax.rem(c - f + nc, nc))
                remote(block, block, xc_s.at[zz, e, f], xc_r.at[zz, e, f], at(z, x, y, cs[f])).wait_recv()

    def finish(zz, way):
        along(zz, way, end)
        relay(zz, way, end)
        across(zz, end)

    cols = q_ref.shape[2] // nz

    def pieces(zz):
        here = pl.ds(pl.multiple_of(zz * cols, cols), cols)
        rest = pl.ds(2 * cols, a_ref.shape[2])
        return (
            (q_ref.at[layer, :, here], w_ref.at[z, x, :, pl.ds(0, cols)]),
            (g_ref.at[layer, :, here], w_ref.at[z, x, :, pl.ds(cols, cols)]),
            (a_ref.at[zz], w_ref.at[z, x, :, rest]),
        )

    def send_own(zz, send, recv, peer):
        for src, dst in pieces(zz):
            remote(src, dst, send, recv, peer).start()
        block = w_ref.at[z, x]
        sent.append(remote(block, block, send, recv, peer))

    def send_w(d):
        send_own(zs[d], wz_s.at[d], wz_r.at[d], at(zs[d], x, y, c))

    def spread_w(src, zz, d):
        for e in range(1, nx):
            copy = remote(src, w_ref.at[zz, x], wx_s.at[d, e], wx_r.at[d, e], at(z, xs[e], y, c))
            copy.start()
            sent.append(copy)

    froms = [lax.rem(z - d + nz, nz) for d in range(nz)]

    def w_arrive(d):
        block = w_ref.at[froms[d], x]
        remote(block, block, wz_s.at[d], wz_r.at[d], at(zs[d], x, y, c)).wait_recv()
        spread_w(block, froms[d], d)

    along(z, 0, begin)
    relay(z, 0, begin)
    for e in range(1, nx):
        send_own(z, wx_s.at[0, e], wx_r.at[0, e], at(z, xs[e], y, c))
    own_rows = pltpu.make_async_copy(x_ref, spot(z, y, c), own_sem.at[0])
    own_rows.start()
    for src, dst in pieces(z):
        pltpu.make_async_copy(src, dst, own_sem.at[1]).start()
    send_w(1)
    for step in range(1, nz):
        visits(z, nz, step, arrive)
        if step + 1 < nz:
            send_w(step + 1)
        w_arrive(step)
    for step in range(nz):
        visits(z, nz, step, from_y)
    for step in range(nz):
        visits(z, nz, step, from_core)
        for e in range(1, nx):
            block = w_ref.at[froms[step], lax.rem(x - e + nx, nx)]
            remote(block, block, wx_s.at[step, e], wx_r.at[step, e], at(z, xs[e], y, c)).wait_recv()
    for step in range(nz):
        visits(z, nz, step, finish)
    for copy in sent:
        copy.wait_send()
    own_rows.wait()
    pltpu.make_async_copy(w_ref.at[z, x], w_ref.at[z, x], own_sem.at[1]).wait()


def gather(nz, nx, ny, nc, layer, ident, rows, query, gate, blocks):
    dma = pltpu.SemaphoreType.DMA
    block = (blocks.shape[1], 2 * query.shape[2] // nz + blocks.shape[2])
    return pl.pallas_call(
        functools.partial(gather_kernel, nz, nx, ny, nc, layer),
        out_shape=(
            jax.ShapeDtypeStruct((nz, ny * nc) + rows.shape, rows.dtype),
            jax.ShapeDtypeStruct((nz, nx) + block, blocks.dtype),
        ),
        in_specs=[
            pl.BlockSpec(memory_space=pltpu.VMEM),
            pl.BlockSpec(memory_space=pl.ANY),
            pl.BlockSpec(memory_space=pl.ANY),
            pl.BlockSpec(memory_space=pltpu.VMEM),
        ],
        out_specs=[pl.BlockSpec(memory_space=pl.ANY)] * 2,
        scratch_shapes=[
            dma((2,)), dma((2, nz)), dma((nz,)), dma((nz, ny)), dma((nz, ny)),
            dma((nz, ny, nc)), dma((nz, ny, nc)), dma((nz,)), dma((nz,)), dma((nz, nx)), dma((nz, nx)),
        ],
        compiler_params=pltpu.CompilerParams(collective_id=ident, has_side_effects=True),
        name="gather" + str(ident),
    )(rows, query, gate, blocks)


def mix_kernel(nz, nx, nc, h_ref, o_ref, all_ref, w_ref, own_sem, hz_s, hz_r, wx_s, wx_r):
    z, x, y, c = place(nx, nc)
    at = lambda zz, xx: (zz * nx + xx, y * nc + c)
    zs = [lax.rem(z + d, nz) for d in range(nz)]
    xs = [lax.rem(x + d, nx) for d in range(nx)]
    greet([at(zs[d], x) for d in range(1, nz)] + [at(z, xs[d]) for d in range(1, nx)])
    wide, deep = h_ref.shape[1], o_ref.shape[1]
    h_at = lambda zz: all_ref.at[:, pl.ds(pl.multiple_of(zz * wide, wide), wide)]
    w_at = lambda xx: w_ref.at[:, pl.ds(pl.multiple_of(xx * deep, deep), deep)]
    along = chain(z, nz, h_at, h_ref, hz_s, hz_r, lambda zz: at(zz, x))
    copies = []
    for e in range(1, nx):
        copies.append(remote(o_ref, w_at(x), wx_s.at[e], wx_r.at[e], at(z, xs[e])))
    copies.append(pltpu.make_async_copy(h_ref, h_at(z), own_sem.at[0]))
    copies.append(pltpu.make_async_copy(o_ref, w_at(x), own_sem.at[1]))
    along(z, 0, lambda copy: copy.start())
    for copy in copies:
        copy.start()

    def arrive(zz, way):
        remote(h_at(zz), h_at(zz), hz_s.at[0, zz], hz_r.at[zz], at(z, x)).wait_recv()
        along(zz, way, lambda copy: copy.start())

    for step in range(1, nz):
        visits(z, nz, step, arrive)
    for copy in copies:
        copy.wait()
    for step in range(nz):
        visits(z, nz, step, lambda zz, way: along(zz, way, lambda copy: copy.wait_send()))


def mix(nz, nx, nc, ident, hidden, out_weight):
    dma = pltpu.SemaphoreType.DMA
    return pl.pallas_call(
        functools.partial(mix_kernel, nz, nx, nc),
        out_shape=(
            jax.ShapeDtypeStruct((hidden.shape[0], hidden.shape[1] * nz), hidden.dtype),
            jax.ShapeDtypeStruct((out_weight.shape[0], out_weight.shape[1] * nx), out_weight.dtype),
        ),
        in_specs=[pl.BlockSpec(memory_space=pltpu.VMEM)] * 2,
        out_specs=[pl.BlockSpec(memory_space=pl.ANY)] * 2,
        scratch_shapes=[dma((2,)), dma((2, nz)), dma((nz,)), dma((nx,)), dma((nx,))],
        compiler_params=pltpu.CompilerParams(collective_id=ident, has_side_effects=True),
        name="mix" + str(ident),
    )(hidden, out_weight)


def settle_kernel(
    nz, nx, ny, nc, p_ref, r_ref, from_c, from_y, out_y, half, whole,
    c_s, c_r, y_s, y_r, z_s, z_r,
):
    z, x, y, c = place(nx, nc)
    at = lambda zz, yy, cc: (zz * nx + x, yy * nc + cc)
    zs = [lax.rem(z + d, nz) for d in range(nz)]
    ys = [lax.rem(y + d, ny) for d in range(ny)]
    cs = [lax.rem(c + d, nc) for d in range(nc)]
    greet(
        [at(zs[d], y, c) for d in range(1, nz)]
        + [at(z, ys[d], c) for d in range(1, ny)]
        + [at(z, y, cs[d]) for d in range(1, nc)]
    )
    order = list(range(1, nz)) + [0]
    far = list(range(1, ny)) + [0]
    sent = []

    def go(*args):
        copy = remote(*args)
        copy.start()
        sent.append(copy)

    for d in order:
        for e in far:
            for f in range(1, nc):
                go(
                    p_ref.at[zs[d], ys[e] * nc + cs[f]], from_c.at[d, e, f],
                    c_s.at[d, e, f], c_r.at[d, e, f], at(z, y, cs[f]),
                )
    for d in order:
        for e in far:
            total = p_ref[zs[d], ys[e] * nc + c]
            for f in range(1, nc):
                part = from_c.at[d, e, f]
                remote(part, part, c_s.at[d, e, f], c_r.at[d, e, f], at(z, y, cs[f])).wait_recv()
                total = total + part[...]
            if e == 0:
                half[d] = total
            else:
                out_y[d, e] = total.astype(out_y.dtype)
                go(out_y.at[d, e], from_y.at[d, e], y_s.at[d, e], y_r.at[d, e], at(z, ys[e], c))
    for d in order:
        total = half[d]
        for e in range(1, ny):
            part = from_y.at[d, e]
            remote(part, part, y_s.at[d, e], y_r.at[d, e], at(z, ys[e], c)).wait_recv()
            total = total + part[...].astype(jnp.float32)
        if d > 0:
            whole[d] = total.astype(whole.dtype)
            go(whole.at[d], r_ref.at[z], z_s.at[d], z_r.at[d], at(zs[d], y, c))
        else:
            r_ref[z] = total.astype(r_ref.dtype)
    for d in range(1, nz):
        block = r_ref.at[lax.rem(z - d + nz, nz)]
        remote(block, block, z_s.at[d], z_r.at[d], at(zs[d], y, c)).wait_recv()
    for copy in sent:
        copy.wait_send()


def settle(nz, nx, ny, nc, ident, partial):
    dma = pltpu.SemaphoreType.DMA
    block = partial.shape[2:]
    return pl.pallas_call(
        functools.partial(settle_kernel, nz, nx, ny, nc),
        out_shape=jax.ShapeDtypeStruct((nz,) + block, jnp.bfloat16),
        in_specs=[pl.BlockSpec(memory_space=pltpu.VMEM)],
        out_specs=pl.BlockSpec(memory_space=pltpu.VMEM),
        scratch_shapes=[
            pltpu.VMEM((nz, ny, nc) + block, partial.dtype),
            pltpu.VMEM((nz, ny) + block, jnp.bfloat16),
            pltpu.VMEM((nz, ny) + block, jnp.bfloat16),
            pltpu.VMEM((nz,) + block, partial.dtype),
            pltpu.VMEM((nz,) + block, jnp.bfloat16),
            dma((nz, ny, nc)), dma((nz, ny, nc)), dma((nz, ny)), dma((nz, ny)), dma((nz,)), dma((nz,)),
        ],
        compiler_params=pltpu.CompilerParams(collective_id=ident, has_side_effects=True),
        name="settle" + str(ident),
    )(partial)


def per_device(
    nz, nx, ny, nc,
    tokens, query_weight, key_weight, value_weight, gate_weight, out_weight, sink_logits, out_gain,
):
    tp_count = ny * nc
    rows_here, width = tokens.shape
    block_rows = rows_here * tp_count
    heads_tp = query_weight.shape[2] // HEAD_DIM
    heads = heads_tp // nz
    cols = heads * HEAD_DIM
    kv = -(-heads // GROUP)
    kv_cols = kv * HEAD_DIM
    per_kv = heads // kv
    z = lax.div(lax.axis_index("sp"), nx)
    x = lax.rem(lax.axis_index("sp"), nx)
    head_start = lax.axis_index("tp") * heads_tp + z * heads

    offset = jnp.arange(WINDOW + block_rows) - WINDOW
    distance = jnp.arange(block_rows)[:, None] - offset[None, :]
    near = (distance >= 0) & (distance < WINDOW)
    start = (jnp.arange(nz) * nx + x) * block_rows
    visible = near[None] & ((start[:, None] + offset[None, :]) >= 0)[:, None, :]
    score_scale = HEAD_DIM ** (-0.5)
    turn = [(a * nx + b, a * nx + (b + 1) % nx) for a in range(nz) for b in range(nx)]

    def arranged(layer):
        parts = []
        for zz in range(nz):
            kv0 = (zz * heads // GROUP) * HEAD_DIM
            parts.append(
                jnp.concatenate(
                    [
                        key_weight[layer, :, kv0 : kv0 + kv_cols],
                        value_weight[layer, :, kv0 : kv0 + kv_cols],
                    ],
                    axis=1,
                )
            )
        return jnp.stack(parts)

    current, result = tokens, None
    for layer in range(LAYERS):
        rows, joined = gather(
            nz, nx, ny, nc, layer, 3 * layer, current, query_weight, gate_weight, arranged(layer)
        )
        rows = rows.reshape(nz * block_rows, width)
        joined = joined.reshape(width, joined.shape[-1])
        projected = jnp.dot(rows, joined, preferred_element_type=jnp.float32).astype(jnp.bfloat16)
        projected = projected.reshape(nz, block_rows, -1)
        own = projected[:, :, 2 * cols :]
        before = lax.ppermute(own[:, -WINDOW:], "sp", turn)
        later = jnp.concatenate([jnp.zeros_like(before[:1]), before[:-1]], axis=0)
        before = jnp.where(x == 0, later, before)
        nearby = jnp.concatenate([before, own], axis=1)
        queries = projected[:, :, :cols].reshape(nz, block_rows, kv, per_kv, HEAD_DIM)
        gate_part = projected[:, :, cols : 2 * cols]
        key_part = nearby[:, :, :kv_cols].reshape(nz, -1, kv, HEAD_DIM)
        value_part = nearby[:, :, kv_cols:].reshape(nz, -1, kv, HEAD_DIM)
        scores = (
            jnp.einsum("bqhgd,bkhd->bhgqk", queries, key_part, preferred_element_type=jnp.float32)
            * score_scale
        )
        scores = jnp.where(visible[:, None, None], scores, masked_score)
        sink = lax.dynamic_slice_in_dim(sink_logits[layer], head_start, heads, 0)
        sink = sink.reshape(1, kv, per_kv, 1, 1)
        highest = jnp.maximum(jnp.max(scores, axis=-1, keepdims=True), sink)
        exponent = jnp.exp(scores - highest)
        weights = (
            exponent / (jnp.sum(exponent, axis=-1, keepdims=True) + jnp.exp(sink - highest))
        ).astype(jnp.bfloat16)
        mixture = jnp.einsum(
            "bhgqk,bkhd->bqhgd", weights, value_part, preferred_element_type=jnp.float32
        ).reshape(nz, block_rows, cols)
        hidden = (mixture * jax.nn.silu(gate_part.astype(jnp.float32))).astype(jnp.bfloat16)
        hidden, out_cols = mix(
            nz, nx, nc, 3 * layer + 1, hidden.reshape(nz * block_rows, cols), out_weight[layer]
        )
        partial_value = jnp.dot(hidden, out_cols, preferred_element_type=jnp.float32)
        partial_value = partial_value.reshape(nz, tp_count, rows_here, -1)
        summed = settle(nz, nx, ny, nc, 3 * layer + 2, partial_value)
        summed = jnp.swapaxes(summed, 0, 1).reshape(rows_here, width).astype(jnp.float32)
        factor = lax.rsqrt(jnp.mean(summed * summed, axis=-1, keepdims=True) + norm_epsilon)
        result = summed * factor * out_gain[layer]
        current = result.astype(jnp.bfloat16)
    return result


def solution(mesh):
    sp, tp = mesh.shape["sp"], mesh.shape["tp"]
    nc = 2 if tp % 2 == 0 else 1
    nx = next(n for n in range(1, sp + 1) if sp % n == 0 and n * n * nc >= sp)
    nz = sp // nx
    placed = (
        P(("sp", "tp"), None),
        P(None, "sp", "tp"),
        P(None, "sp", "tp"),
        P(None, "sp", "tp"),
        P(None, "sp", "tp"),
        P(None, "tp", "sp"),
        P(),
        P(),
    )
    return jax.shard_map(
        functools.partial(per_device, nz, nx, tp // nc, nc),
        mesh=mesh, in_specs=placed, out_specs=P(("sp", "tp"), None), check_vma=False,
    )
```

```python
import functools

import jax
import jax.numpy as jnp
from jax import lax
from jax.experimental import pallas as pl
from jax.experimental.pallas import tpu as pltpu
from jax.sharding import PartitionSpec as P

HEAD_DIM = 64
WINDOW = 128
LAYERS = 2
GROUP = 8

norm_epsilon = 1e-05
masked_score = -1e30
MESH = pl.DeviceIdType.MESH


def place(nx, ncore):
    sp, tp = lax.axis_index("sp"), lax.axis_index("tp")
    return lax.div(sp, nx), lax.rem(sp, nx), lax.div(tp, ncore), lax.rem(tp, ncore)


def greet(peers):
    barrier = pltpu.get_barrier_semaphore()
    for peer in peers:
        pl.semaphore_signal(barrier, inc=1, device_id=peer, device_id_type=MESH)
    pl.semaphore_wait(barrier, len(peers))


def remote(src, dst, send, recv, peer):
    return pltpu.make_async_remote_copy(
        src_ref=src, dst_ref=dst, send_sem=send, recv_sem=recv, device_id=peer, device_id_type=MESH
    )


def visits(z, nz, step, act):
    if step == 0:
        act(z, 0)
        return
    pl.when(z >= step)(lambda: act(z - step, 1))
    pl.when(z + step < nz)(lambda: act(z + step, -1))


def chain(z, nz, block, own, send, recv, peer):
    def both(zz, way, use):
        if way >= 0:
            src = own if way == 0 else block(zz)
            copy = remote(src, block(zz), send.at[0, zz], recv.at[zz], peer(z + 1))
            pl.when(z + 1 < nz)(lambda: use(copy))
        if way <= 0:
            src = own if way == 0 else block(zz)
            copy_down = remote(src, block(zz), send.at[1, zz], recv.at[zz], peer(z - 1))
            pl.when(z >= 1)(lambda: use(copy_down))

    return both


def gather_kernel(
    nz, nx, ny, nc, layer, x_ref, q_ref, g_ref, a_ref, rows_ref, w_ref,
    own_sem, xz_s, xz_r, xy_s, xy_r, xc_s, xc_r, wz_s, wz_r, wx_s, wx_r,
):
    z, x, y, c = place(nx, nc)
    at = lambda zz, xx, yy, cc: (zz * nx + xx, yy * nc + cc)
    zs = [lax.rem(z + d, nz) for d in range(nz)]
    xs = [lax.rem(x + d, nx) for d in range(nx)]
    ys = [lax.rem(y + d, ny) for d in range(ny)]
    cs = [lax.rem(c + d, nc) for d in range(nc)]
    greet(
        [at(zs[d], x, y, c) for d in range(1, nz)]
        + [at(z, xs[d], y, c) for d in range(1, nx)]
        + [at(z, x, ys[d], c) for d in range(1, ny)]
        + [at(z, x, y, cs[d]) for d in range(1, nc)]
    )
    sent = []
    begin = lambda copy: copy.start()
    end = lambda copy: copy.wait_send()
    spot = lambda zz, yy, cc: rows_ref.at[zz, yy * nc + cc]
    along = chain(z, nz, lambda zz: spot(zz, y, c), x_ref, xz_s, xz_r, lambda zz: at(zz, x, y, c))

    def relay(zz, way, use):
        src = x_ref if way == 0 else spot(zz, y, c)
        for e in range(1, ny):
            use(remote(src, spot(zz, y, c), xy_s.at[zz, e], xy_r.at[zz, e], at(z, x, ys[e], c)))
        for f in range(1, nc):
            use(remote(src, spot(zz, y, c), xc_s.at[zz, 0, f], xc_r.at[zz, 0, f], at(z, x, y, cs[f])))

    def across(zz, use):
        for e in range(1, ny):
            block = spot(zz, lax.rem(y - e + ny, ny), c)
            for f in range(1, nc):
                use(remote(block, block, xc_s.at[zz, e, f], xc_r.at[zz, e, f], at(z, x, y, cs[f])))

    def arrive(zz, way):
        block = spot(zz, y, c)
        remote(block, block, xz_s.at[0, zz], xz_r.at[zz], at(z, x, y, c)).wait_recv()
        along(zz, way, begin)
        relay(zz, way, begin)

    def from_y(zz, way):
        for e in range(1, ny):
            block = spot(zz, lax.rem(y - e + ny, ny), c)
            remote(block, block, xy_s.at[zz, e], xy_r.at[zz, e], at(z, x, ys[e], c)).wait_recv()
        across(zz, begin)

    def from_core(zz, way):
        for e in range(ny):
            for f in range(1, nc):
                block = spot(zz, lax.rem(y - e + ny, ny), lax.rem(c - f + nc, nc))
                remote(block, block, xc_s.at[zz, e, f], xc_r.at[zz, e, f], at(z, x, y, cs[f])).wait_recv()

    def finish(zz, way):
        along(zz, way, end)
        relay(zz, way, end)
        across(zz, end)

    cols = q_ref.shape[2] // nz

    def pieces(zz):
        here = pl.ds(pl.multiple_of(zz * cols, cols), cols)
        rest = pl.ds(2 * cols, a_ref.shape[2])
        return (
            (q_ref.at[layer, :, here], w_ref.at[z, x, :, pl.ds(0, cols)]),
            (g_ref.at[layer, :, here], w_ref.at[z, x, :, pl.ds(cols, cols)]),
            (a_ref.at[zz], w_ref.at[z, x, :, rest]),
        )

    def send_own(zz, send, recv, peer):
        for src, dst in pieces(zz):
            remote(src, dst, send, recv, peer).start()
        block = w_ref.at[z, x]
        sent.append(remote(block, block, send, recv, peer))

    def send_w(d):
        send_own(zs[d], wz_s.at[d], wz_r.at[d], at(zs[d], x, y, c))

    def spread_w(src, zz, d):
        for e in range(1, nx):
            copy = remote(src, w_ref.at[zz, x], wx_s.at[d, e], wx_r.at[d, e], at(z, xs[e], y, c))
            copy.start()
            sent.append(copy)

    froms = [lax.rem(z - d + nz, nz) for d in range(nz)]

    def w_arrive(d):
        block = w_ref.at[froms[d], x]
        remote(block, block, wz_s.at[d], wz_r.at[d], at(zs[d], x, y, c)).wait_recv()
        spread_w(block, froms[d], d)

    along(z, 0, begin)
    relay(z, 0, begin)
    for e in range(1, nx):
        send_own(z, wx_s.at[0, e], wx_r.at[0, e], at(z, xs[e], y, c))
    own_rows = pltpu.make_async_copy(x_ref, spot(z, y, c), own_sem.at[0])
    own_rows.start()
    for src, dst in pieces(z):
        pltpu.make_async_copy(src, dst, own_sem.at[1]).start()
    for step in range(1, nz):
        send_w(step)
    for step in range(1, nz):
        visits(z, nz, step, arrive)
        w_arrive(step)
    for step in range(nz):
        visits(z, nz, step, from_y)
    for step in range(nz):
        visits(z, nz, step, from_core)
        for e in range(1, nx):
            block = w_ref.at[froms[step], lax.rem(x - e + nx, nx)]
            remote(block, block, wx_s.at[step, e], wx_r.at[step, e], at(z, xs[e], y, c)).wait_recv()
    for step in range(nz):
        visits(z, nz, step, finish)
    for copy in sent:
        copy.wait_send()
    own_rows.wait()
    pltpu.make_async_copy(w_ref.at[z, x], w_ref.at[z, x], own_sem.at[1]).wait()


def gather(nz, nx, ny, nc, layer, ident, rows, query, gate, blocks):
    dma = pltpu.SemaphoreType.DMA
    block = (blocks.shape[1], 2 * query.shape[2] // nz + blocks.shape[2])
    return pl.pallas_call(
        functools.partial(gather_kernel, nz, nx, ny, nc, layer),
        out_shape=(
            jax.ShapeDtypeStruct((nz, ny * nc) + rows.shape, rows.dtype),
            jax.ShapeDtypeStruct((nz, nx) + block, blocks.dtype),
        ),
        in_specs=[
            pl.BlockSpec(memory_space=pltpu.VMEM),
            pl.BlockSpec(memory_space=pl.ANY),
            pl.BlockSpec(memory_space=pl.ANY),
            pl.BlockSpec(memory_space=pltpu.VMEM),
        ],
        out_specs=[pl.BlockSpec(memory_space=pl.ANY)] * 2,
        scratch_shapes=[
            dma((2,)), dma((2, nz)), dma((nz,)), dma((nz, ny)), dma((nz, ny)),
            dma((nz, ny, nc)), dma((nz, ny, nc)), dma((nz,)), dma((nz,)), dma((nz, nx)), dma((nz, nx)),
        ],
        compiler_params=pltpu.CompilerParams(collective_id=ident, has_side_effects=True),
        name="gather" + str(ident),
    )(rows, query, gate, blocks)


def mix_kernel(nz, nx, nc, h_ref, o_ref, all_ref, w_ref, own_sem, hz_s, hz_r, wx_s, wx_r):
    z, x, y, c = place(nx, nc)
    at = lambda zz, xx: (zz * nx + xx, y * nc + c)
    zs = [lax.rem(z + d, nz) for d in range(nz)]
    xs = [lax.rem(x + d, nx) for d in range(nx)]
    greet([at(zs[d], x) for d in range(1, nz)] + [at(z, xs[d]) for d in range(1, nx)])
    wide, deep = h_ref.shape[1], o_ref.shape[1]
    h_at = lambda zz: all_ref.at[:, pl.ds(pl.multiple_of(zz * wide, wide), wide)]
    w_at = lambda xx: w_ref.at[:, pl.ds(pl.multiple_of(xx * deep, deep), deep)]
    along = chain(z, nz, h_at, h_ref, hz_s, hz_r, lambda zz: at(zz, x))
    copies = []
    for e in range(1, nx):
        copies.append(remote(o_ref, w_at(x), wx_s.at[e], wx_r.at[e], at(z, xs[e])))
    copies.append(pltpu.make_async_copy(h_ref, h_at(z), own_sem.at[0]))
    copies.append(pltpu.make_async_copy(o_ref, w_at(x), own_sem.at[1]))
    along(z, 0, lambda copy: copy.start())
    for copy in copies:
        copy.start()

    def arrive(zz, way):
        remote(h_at(zz), h_at(zz), hz_s.at[0, zz], hz_r.at[zz], at(z, x)).wait_recv()
        along(zz, way, lambda copy: copy.start())

    for step in range(1, nz):
        visits(z, nz, step, arrive)
    for copy in copies:
        copy.wait()
    for step in range(nz):
        visits(z, nz, step, lambda zz, way: along(zz, way, lambda copy: copy.wait_send()))


def mix(nz, nx, nc, ident, hidden, out_weight):
    dma = pltpu.SemaphoreType.DMA
    return pl.pallas_call(
        functools.partial(mix_kernel, nz, nx, nc),
        out_shape=(
            jax.ShapeDtypeStruct((hidden.shape[0], hidden.shape[1] * nz), hidden.dtype),
            jax.ShapeDtypeStruct((out_weight.shape[0], out_weight.shape[1] * nx), out_weight.dtype),
        ),
        in_specs=[pl.BlockSpec(memory_space=pltpu.VMEM)] * 2,
        out_specs=[pl.BlockSpec(memory_space=pl.ANY)] * 2,
        scratch_shapes=[dma((2,)), dma((2, nz)), dma((nz,)), dma((nx,)), dma((nx,))],
        compiler_params=pltpu.CompilerParams(collective_id=ident, has_side_effects=True),
        name="mix" + str(ident),
    )(hidden, out_weight)


def settle_kernel(
    nz, nx, ny, nc, p_ref, r_ref, from_c, from_y, out_y, half, whole,
    c_s, c_r, y_s, y_r, z_s, z_r,
):
    z, x, y, c = place(nx, nc)
    at = lambda zz, yy, cc: (zz * nx + x, yy * nc + cc)
    zs = [lax.rem(z + d, nz) for d in range(nz)]
    ys = [lax.rem(y + d, ny) for d in range(ny)]
    cs = [lax.rem(c + d, nc) for d in range(nc)]
    greet(
        [at(zs[d], y, c) for d in range(1, nz)]
        + [at(z, ys[d], c) for d in range(1, ny)]
        + [at(z, y, cs[d]) for d in range(1, nc)]
    )
    order = list(range(1, nz)) + [0]
    far = list(range(1, ny)) + [0]
    sent = []

    def go(*args):
        copy = remote(*args)
        copy.start()
        sent.append(copy)

    for d in order:
        for e in far:
            for f in range(1, nc):
                go(
                    p_ref.at[zs[d], ys[e] * nc + cs[f]], from_c.at[d, e, f],
                    c_s.at[d, e, f], c_r.at[d, e, f], at(z, y, cs[f]),
                )
    for d in order:
        for e in far:
            total = p_ref[zs[d], ys[e] * nc + c]
            for f in range(1, nc):
                part = from_c.at[d, e, f]
                remote(part, part, c_s.at[d, e, f], c_r.at[d, e, f], at(z, y, cs[f])).wait_recv()
                total = total + part[...]
            if e == 0:
                half[d] = total
            else:
                out_y[d, e] = total.astype(out_y.dtype)
                go(out_y.at[d, e], from_y.at[d, e], y_s.at[d, e], y_r.at[d, e], at(z, ys[e], c))
    for d in order:
        total = half[d]
        for e in range(1, ny):
            part = from_y.at[d, e]
            remote(part, part, y_s.at[d, e], y_r.at[d, e], at(z, ys[e], c)).wait_recv()
            total = total + part[...].astype(jnp.float32)
        if d > 0:
            whole[d] = total.astype(whole.dtype)
            go(whole.at[d], r_ref.at[z], z_s.at[d], z_r.at[d], at(zs[d], y, c))
        else:
            r_ref[z] = total.astype(r_ref.dtype)
    for d in range(1, nz):
        block = r_ref.at[lax.rem(z - d + nz, nz)]
        remote(block, block, z_s.at[d], z_r.at[d], at(zs[d], y, c)).wait_recv()
    for copy in sent:
        copy.wait_send()


def settle(nz, nx, ny, nc, ident, partial):
    dma = pltpu.SemaphoreType.DMA
    block = partial.shape[2:]
    return pl.pallas_call(
        functools.partial(settle_kernel, nz, nx, ny, nc),
        out_shape=jax.ShapeDtypeStruct((nz,) + block, jnp.bfloat16),
        in_specs=[pl.BlockSpec(memory_space=pltpu.VMEM)],
        out_specs=pl.BlockSpec(memory_space=pltpu.VMEM),
        scratch_shapes=[
            pltpu.VMEM((nz, ny, nc) + block, partial.dtype),
            pltpu.VMEM((nz, ny) + block, jnp.bfloat16),
            pltpu.VMEM((nz, ny) + block, jnp.bfloat16),
            pltpu.VMEM((nz,) + block, partial.dtype),
            pltpu.VMEM((nz,) + block, jnp.bfloat16),
            dma((nz, ny, nc)), dma((nz, ny, nc)), dma((nz, ny)), dma((nz, ny)), dma((nz,)), dma((nz,)),
        ],
        compiler_params=pltpu.CompilerParams(collective_id=ident, has_side_effects=True),
        name="settle" + str(ident),
    )(partial)


def per_device(
    nz, nx, ny, nc,
    tokens, query_weight, key_weight, value_weight, gate_weight, out_weight, sink_logits, out_gain,
):
    tp_count = ny * nc
    rows_here, width = tokens.shape
    block_rows = rows_here * tp_count
    heads_tp = query_weight.shape[2] // HEAD_DIM
    heads = heads_tp // nz
    cols = heads * HEAD_DIM
    kv = -(-heads // GROUP)
    kv_cols = kv * HEAD_DIM
    per_kv = heads // kv
    z = lax.div(lax.axis_index("sp"), nx)
    x = lax.rem(lax.axis_index("sp"), nx)
    head_start = lax.axis_index("tp") * heads_tp + z * heads

    offset = jnp.arange(WINDOW + block_rows) - WINDOW
    distance = jnp.arange(block_rows)[:, None] - offset[None, :]
    near = (distance >= 0) & (distance < WINDOW)
    start = (jnp.arange(nz) * nx + x) * block_rows
    visible = near[None] & ((start[:, None] + offset[None, :]) >= 0)[:, None, :]
    score_scale = HEAD_DIM ** (-0.5)
    turn = [(a * nx + b, a * nx + (b + 1) % nx) for a in range(nz) for b in range(nx)]

    def arranged(layer):
        parts = []
        for zz in range(nz):
            kv0 = (zz * heads // GROUP) * HEAD_DIM
            parts.append(
                jnp.concatenate(
                    [
                        key_weight[layer, :, kv0 : kv0 + kv_cols],
                        value_weight[layer, :, kv0 : kv0 + kv_cols],
                    ],
                    axis=1,
                )
            )
        return jnp.stack(parts)

    current, result = tokens, None
    for layer in range(LAYERS):
        rows, joined = gather(
            nz, nx, ny, nc, layer, 3 * layer, current, query_weight, gate_weight, arranged(layer)
        )
        rows = rows.reshape(nz * block_rows, width)
        joined = joined.reshape(width, joined.shape[-1])
        projected = jnp.dot(rows, joined, preferred_element_type=jnp.float32).astype(jnp.bfloat16)
        projected = projected.reshape(nz, block_rows, -1)
        own = projected[:, :, 2 * cols :]
        before = lax.ppermute(own[:, -WINDOW:], "sp", turn)
        later = jnp.concatenate([jnp.zeros_like(before[:1]), before[:-1]], axis=0)
        before = jnp.where(x == 0, later, before)
        nearby = jnp.concatenate([before, own], axis=1)
        queries = projected[:, :, :cols].reshape(nz, block_rows, kv, per_kv, HEAD_DIM)
        gate_part = projected[:, :, cols : 2 * cols]
        key_part = nearby[:, :, :kv_cols].reshape(nz, -1, kv, HEAD_DIM)
        value_part = nearby[:, :, kv_cols:].reshape(nz, -1, kv, HEAD_DIM)
        scores = (
            jnp.einsum("bqhgd,bkhd->bhgqk", queries, key_part, preferred_element_type=jnp.float32)
            * score_scale
        )
        scores = jnp.where(visible[:, None, None], scores, masked_score)
        sink = lax.dynamic_slice_in_dim(sink_logits[layer], head_start, heads, 0)
        sink = sink.reshape(1, kv, per_kv, 1, 1)
        highest = jnp.maximum(jnp.max(scores, axis=-1, keepdims=True), sink)
        exponent = jnp.exp(scores - highest)
        weights = (
            exponent / (jnp.sum(exponent, axis=-1, keepdims=True) + jnp.exp(sink - highest))
        ).astype(jnp.bfloat16)
        mixture = jnp.einsum(
            "bhgqk,bkhd->bqhgd", weights, value_part, preferred_element_type=jnp.float32
        ).reshape(nz, block_rows, cols)
        hidden = (mixture * jax.nn.silu(gate_part.astype(jnp.float32))).astype(jnp.bfloat16)
        hidden, out_cols = mix(
            nz, nx, nc, 3 * layer + 1, hidden.reshape(nz * block_rows, cols), out_weight[layer]
        )
        partial_value = jnp.dot(hidden, out_cols, preferred_element_type=jnp.float32)
        partial_value = partial_value.reshape(nz, tp_count, rows_here, -1)
        summed = settle(nz, nx, ny, nc, 3 * layer + 2, partial_value)
        summed = jnp.swapaxes(summed, 0, 1).reshape(rows_here, width).astype(jnp.float32)
        factor = lax.rsqrt(jnp.mean(summed * summed, axis=-1, keepdims=True) + norm_epsilon)
        result = summed * factor * out_gain[layer]
        current = result.astype(jnp.bfloat16)
    return result


def solution(mesh):
    sp, tp = mesh.shape["sp"], mesh.shape["tp"]
    nc = 2 if tp % 2 == 0 else 1
    nx = next(n for n in range(1, sp + 1) if sp % n == 0 and n * n * nc >= sp)
    nz = sp // nx
    placed = (
        P(("sp", "tp"), None),
        P(None, "sp", "tp"),
        P(None, "sp", "tp"),
        P(None, "sp", "tp"),
        P(None, "sp", "tp"),
        P(None, "tp", "sp"),
        P(),
        P(),
    )
    return jax.shard_map(
        functools.partial(per_device, nz, nx, tp // nc, nc),
        mesh=mesh, in_specs=placed, out_specs=P(("sp", "tp"), None), check_vma=False,
    )
```
